32 devices in a mesh: fs: 4 (over z), rep: 4 (over y, x), tp: 2 (over core).
Axes of the slice: x: 2, y: 2, z: 4, core: 2. Of those that a mesh axis runs over, the one named last changes fastest.
Arguments:
- normed_input: bfloat16 [4096, 2048], P(('fs', 'rep')), may hold values from -20 to 20
- key_cotangent: bfloat16 [4096, 2048], P(('fs', 'rep'), 'tp'), may hold values from -0.03125 to 0.03125
- value_cotangent: bfloat16 [4096, 4096], P(('fs', 'rep'), 'tp'), may hold values from -0.03125 to 0.03125
- key_basis: bfloat16 [2048, 256], P('tp'), may hold values from -0.375 to 0.375
- value_basis: bfloat16 [4096, 256], P('tp'), may hold values from -0.375 to 0.375
- key_master: float32 [2048, 2048], P('fs', 'tp'), may hold values from -0.125 to 0.125
- value_master: float32 [2048, 4096], P('fs', 'tp'), may hold values from -0.125 to 0.125
- key_moment: float32 [2048, 256], P(('fs', 'rep'), 'tp'), may hold values from -200 to 200
- key_second: float32 [2048, 256], P(('fs', 'rep'), 'tp'), may hold values from 0.05 to 0.5
- value_moment: float32 [2048, 256], P(('fs', 'rep'), 'tp'), may hold values from -200 to 200
- value_second: float32 [2048, 256], P(('fs', 'rep'), 'tp'), may hold values from 0.05 to 0.5
Outputs:
- key_mean: float32 [2048, 256], P(('fs', 'rep'), 'tp')
- key_square: float32 [2048, 256], P(('fs', 'rep'), 'tp')
- value_mean: float32 [2048, 256], P(('fs', 'rep'), 'tp')
- value_square: float32 [2048, 256], P(('fs', 'rep'), 'tp')
- key_step: float32 [2048, 2048], P('fs', 'tp')
- value_step: float32 [2048, 4096], P('fs', 'tp')
- key_weight: bfloat16 [2048, 2048], P('fs', 'tp')
- value_weight: bfloat16 [2048, 4096], P('fs', 'tp')
The draws below stay inside these ranges and needn't reach their ends.
All inputs are finite; a program needn't handle non-finite values.
Results may differ from the reference program's by a relative error of at most 0.0034.
Values may be sent and summed in bfloat16 or wider, within the bound.
A program may use at most 64 MiB of HBM per device.

```python
import math
import jax
import jax.numpy as jnp
from jax import lax

D = 2048
HEADS = 8
DK = 256
DV = 512
RANK = 256
TOK_DEV = 256
KEY_WIDTH = 2048
VALUE_WIDTH = 4096
TOKENS = 4096


def moment_draw(key, rows, cols):
    base = jnp.clip(jax.random.normal(jax.random.fold_in(key, 11), (rows, cols), jnp.float32), -4.0, 4.0)
    position = jnp.arange(rows, dtype=jnp.float32) / (rows - 1)
    col_scale = jnp.exp(jax.random.uniform(jax.random.fold_in(key, 12), (cols,), jnp.float32) * jnp.log(10.0))
    row_scale = jnp.exp(position * jnp.log(10.0))
    return 0.1 * base * row_scale[:, None] * col_scale[None, :]


def draw_key_moment(key, part):
    return moment_draw(jax.random.fold_in(key, 1), D, RANK)


def draw_value_moment(key, part):
    return moment_draw(jax.random.fold_in(key, 2), D, RANK)


def token_sign(key):
    flips = jax.random.randint(jax.random.fold_in(key, 500), (TOKENS,), 0, 2)
    return (2 * flips - 1).astype(jnp.float32)


def noise_draw(key, rows, cols):
    return jnp.clip(jax.random.normal(key, (rows, cols), jnp.float32), -6.0, 6.0)


def shared_part(key, salt, cols):
    amplitude = 1.4142 / TOKENS ** 0.25
    pattern = jnp.clip(jax.random.normal(jax.random.fold_in(key, salt), (cols,), jnp.float32), -4.0, 4.0)
    return amplitude * token_sign(key)[:, None] * pattern[None, :]


def draw_normed_input(key, part):
    noise = noise_draw(jax.random.fold_in(key, 21), TOKENS, D)
    blocks = TOKENS // TOK_DEV
    pairing = jax.random.permutation(jax.random.fold_in(key, 22), blocks)
    token_block = jnp.arange(TOKENS, dtype=jnp.int32) // TOK_DEV
    partner = pairing[token_block]
    feature_block = jnp.arange(D, dtype=jnp.int32) // (D // blocks)
    boost = jnp.where(partner[:, None] == feature_block[None, :], 3.0, 1.0)
    values = boost * noise + shared_part(key, 23, D)
    return values.astype(jnp.bfloat16)


def draw_key_cotangent(key, part):
    noise = noise_draw(jax.random.fold_in(key, 31), TOKENS, HEADS * DK)
    values = 0.25 / TOKENS ** 0.5 * (noise + shared_part(key, 33, HEADS * DK))
    return values.astype(jnp.bfloat16)


def draw_value_cotangent(key, part):
    noise = noise_draw(jax.random.fold_in(key, 41), TOKENS, HEADS * DV)
    values = 0.25 / TOKENS ** 0.5 * (noise + shared_part(key, 43, HEADS * DV))
    return values.astype(jnp.bfloat16)


def levels(key, extent, split, smallest, high):
    loudness, own = 1.0, jax.random.fold_in(key, 6)
    for axis_at, blocks in split:
        draws = jnp.exp(jax.random.uniform(jax.random.fold_in(own, axis_at), (blocks,), jnp.float32, smallest / len(split), high / len(split)))
        loudness = loudness * jnp.repeat(draws, extent[axis_at] // blocks).reshape([-1 if axis == axis_at else 1 for axis in range(len(extent))])
    return loudness


def gaussian(stream_key, shape, deviation, most, split=(), kind=jnp.bfloat16):
    loudness = levels(stream_key, shape, split, -0.22, 0.18) if split else 1.0
    values = jax.random.normal(stream_key, shape, jnp.float32) * deviation * loudness
    return jnp.minimum(jnp.maximum(values, -most), most).astype(kind)


def setup_inputs(seed: int = 0) -> dict:
    keys = jax.random.split(jax.random.key(seed), 12)
    return {
        "normed_input": draw_normed_input(jax.random.fold_in(keys[11], 71), 0),
        "key_cotangent": draw_key_cotangent(jax.random.fold_in(keys[11], 71), 0),
        "value_cotangent": draw_value_cotangent(jax.random.fold_in(keys[11], 71), 0),
        "key_basis": gaussian(keys[3], (KEY_WIDTH, RANK), RANK ** -0.5, 0.375, ((0, 2),)),
        "value_basis": gaussian(keys[4], (VALUE_WIDTH, RANK), RANK ** -0.5, 0.375, ((0, 2),)),
        "key_master": gaussian(keys[5], (D, KEY_WIDTH), D ** -0.5, 0.125, ((0, 4), (1, 2)), jnp.float32),
        "value_master": gaussian(keys[6], (D, VALUE_WIDTH), D ** -0.5, 0.125, ((0, 4), (1, 2)), jnp.float32),
        "key_moment": draw_key_moment(jax.random.fold_in(keys[11], 71), 0),
        "key_second": jnp.clip(jnp.exp(math.log(0.5) - 2.3025851 * jax.random.uniform(keys[8], (D, RANK), jnp.float32) ** levels(keys[8], (D, RANK), ((0, 16), (1, 2)), -0.2, 0.2)), 0.05, 0.5),
        "value_moment": draw_value_moment(jax.random.fold_in(keys[11], 71), 0),
        "value_second": jnp.clip(jnp.exp(math.log(0.5) - 2.3025851 * jax.random.uniform(keys[10], (D, RANK), jnp.float32) ** levels(keys[10], (D, RANK), ((0, 16), (1, 2)), -0.2, 0.2)), 0.05, 0.5),
    }


first_decay = 0.8
second_decay = 0.9
root_epsilon = 1e-08
mean_epsilon = 1e-06
learn_rate = 0.01

def reference(normed_input, key_cotangent, value_cotangent, key_basis, value_basis, key_master, value_master, key_moment, key_second, value_moment, value_second):
    key_proj = jnp.dot(key_cotangent, key_basis, preferred_element_type=jnp.float32).astype(jnp.bfloat16)
    value_proj = jnp.dot(value_cotangent, value_basis, preferred_element_type=jnp.float32).astype(jnp.bfloat16)
    joined = jnp.concatenate([key_proj, value_proj], axis=1)
    summed = jnp.dot(normed_input.T, joined, preferred_element_type=jnp.float32)
    key_grad = summed[:, :RANK]
    value_grad = summed[:, RANK:]
    key_mean = first_decay * key_moment + (1.0 - first_decay) * key_grad
    value_mean = first_decay * value_moment + (1.0 - first_decay) * value_grad
    key_square = second_decay * key_second + (1.0 - second_decay) * key_grad * key_grad
    value_square = second_decay * value_second + (1.0 - second_decay) * value_grad * value_grad
    key_ratio = key_mean / (jnp.sqrt(key_square) + root_epsilon)
    value_ratio = value_mean / (jnp.sqrt(value_square) + root_epsilon)
    total = jnp.sum(key_ratio * key_ratio) + jnp.sum(value_ratio * value_ratio)
    scale = jnp.sqrt(total / (2 * D * RANK) + mean_epsilon)
    key_dir = (key_ratio / scale).astype(jnp.bfloat16)
    value_dir = (value_ratio / scale).astype(jnp.bfloat16)
    dims = (((1,), (1,)), ((), ()))
    key_step = lax.dot_general(key_dir, key_basis, dims, preferred_element_type=jnp.float32)
    value_step = lax.dot_general(value_dir, value_basis, dims, preferred_element_type=jnp.float32)
    key_weight = (key_master - learn_rate * key_step).astype(jnp.bfloat16)
    value_weight = (value_master - learn_rate * value_step).astype(jnp.bfloat16)
    return (key_mean, key_square, value_mean, value_square, key_step, value_step, key_weight, value_weight)
```

```python
import functools

import jax
import jax.numpy as jnp
from jax import lax
from jax.experimental import pallas as pl
from jax.experimental.pallas import tpu as pltpu
from jax.sharding import PartitionSpec as P

first_decay = 0.8
second_decay = 0.9
root_epsilon = 1e-08
mean_epsilon = 1e-06
learn_rate = 0.01

F32 = jnp.float32
BF16 = jnp.bfloat16
MESH = pl.DeviceIdType.MESH


def moments(grad, moment, second):
    mean = first_decay * moment + (1.0 - first_decay) * grad
    square = second_decay * second + (1.0 - second_decay) * grad * grad
    return mean, square


def remote(src, dst, send, recv, where):
    return pltpu.make_async_remote_copy(
        src_ref=src, dst_ref=dst, send_sem=send, recv_sem=recv,
        device_id=where, device_id_type=MESH,
    )


def exchange(
    F, R,
    x, kc, vc, kb, vb, km, ks, vm, vs,
    gath, total, grad,
    x_v, kc_v, vc_v, kb_v, vb_v, km_v, ks_v, vm_v, vs_v,
    proj, proj_in, part, land1, out2, land2, sq1, sq2,
    load, p_send, p_recv, s1, r1, s2, r2, gs, gr, fs_, fr, q1s, q1r, q2s, q2r,
):
    f0, r0, t0 = lax.axis_index("fs"), lax.axis_index("rep"), lax.axis_index("tp")
    t1 = 1 - t0
    D = x.shape[1]
    rows, width = km.shape
    wire = part.dtype

    pairs = [(kc, kc_v), (kb, kb_v), (vc, vc_v), (vb, vb_v), (x, x_v),
             (km, km_v), (ks, ks_v), (vm, vm_v), (vs, vs_v)]
    loads = [pltpu.make_async_copy(a, b, load.at[i]) for i, (a, b) in enumerate(pairs)]
    for c in loads:
        c.start()

    barrier = pltpu.get_barrier_semaphore()

    def greet_fs(d, _):
        pl.semaphore_signal(barrier, inc=1, device_id={"fs": lax.rem(f0 + d, F)}, device_id_type=MESH)
        return 0

    lax.fori_loop(1, F, greet_fs, 0)
    group = [(k, t) for k in range(R) for t in range(2) if (k, t) != (0, 0)]
    for k, t in group:
        pl.semaphore_signal(
            barrier, inc=1,
            device_id={"rep": lax.rem(r0 + k, R), "tp": lax.rem(t0 + t, 2)},
            device_id_type=MESH,
        )

    for c in loads[:2]:
        c.wait()
    pk = jnp.dot(kc_v[...], kb_v[...], preferred_element_type=F32)
    for t in range(2):
        proj[t, :, :width] = pk[:, t * width:(t + 1) * width]
    for c in loads[2:4]:
        c.wait()
    pv = jnp.dot(vc_v[...], vb_v[...], preferred_element_type=F32)
    for t in range(2):
        proj[t, :, width:] = pv[:, t * width:(t + 1) * width]

    pl.semaphore_wait(barrier, F - 1 + 2 * R - 1)
    swap = remote(proj.at[t1], proj_in, p_send, p_recv, {"tp": t1})
    swap.start()
    loads[4].wait()
    swap.wait_recv()
    joined = (proj[t0] + proj_in[...]).astype(BF16)

    tile = min(256, D)
    for i in range(D // tile):
        g = lax.dot_general(
            x_v[:, i * tile:(i + 1) * tile], joined, (((0,), (0,)), ((), ())),
            preferred_element_type=F32,
        )
        for c in range(tile // rows):
            at = i * (tile // rows) + c
            part[at // R, at % R] = g[c * rows:(c + 1) * rows].astype(wire)

    def copy1(f, k):
        r = lax.rem(r0 + k, R)
        return remote(part.at[f, r], land1.at[f, r0], s1.at[f, r], r1.at[f, r0], {"rep": r})

    def wait1(f, k):
        r = lax.rem(r0 + k, R)
        remote(part.at[f, r], land1.at[f, r], s1.at[f, r], r1.at[f, r], {"rep": r}).wait_recv()

    def send1(d, _):
        f = lax.rem(f0 + d, F)
        for k in range(1, R):
            copy1(f, k).start()
        return 0

    lax.fori_loop(1, F + 1, send1, 0)

    def gather1(f):
        acc = part[f, r0].astype(F32)
        for k in range(1, R):
            wait1(f, k)
            acc = acc + land1[f, lax.rem(r0 + k, R)].astype(F32)
        return acc

    def send2(d, _):
        f = lax.rem(f0 + d, F)
        out2[f] = gather1(f).astype(wire)
        remote(out2.at[f], land2.at[f0], s2.at[f], r2.at[f0], {"fs": f}).start()
        return 0

    lax.fori_loop(1, F, send2, 0)
    for c in loads[5:]:
        c.wait()
    grad[...] = gather1(f0)

    def add2(d, _):
        f = lax.rem(f0 + d, F)
        remote(out2.at[f], land2.at[f], s2.at[f], r2.at[f], {"fs": f}).wait_recv()
        grad[...] += land2[f].astype(F32)
        return 0

    lax.fori_loop(1, F, add2, 0)

    squares = 0.0
    for h, (m_v, s_v) in enumerate(((km_v, ks_v), (vm_v, vs_v))):
        mean, square = moments(grad[:, h * width:(h + 1) * width], m_v[...], s_v[...])
        ratio = mean / (jnp.sqrt(square) + root_epsilon)
        gath[t0, r0, :, h * width:(h + 1) * width] = ratio.astype(BF16)
        squares = squares + jnp.sum(ratio * ratio, axis=0, keepdims=True)
    sq1[f0] = squares

    def sq1_copy(d):
        f = lax.rem(f0 + d, F)
        return remote(sq1.at[f0], sq1.at[f0], q1s.at[f], q1r.at[f0], {"fs": f})

    def sq1_wait(d, acc):
        f = lax.rem(f0 + d, F)
        remote(sq1.at[f], sq1.at[f], q1s.at[f], q1r.at[f], {"fs": f}).wait_recv()
        return acc

    def sq1_start(d, _):
        sq1_copy(d).start()
        return 0

    lax.fori_loop(1, F, sq1_start, 0)

    for k in range(1, R):
        r = lax.rem(r0 + k, R)
        remote(gath.at[t0, r0], gath.at[t0, r0], gs.at[r], gr.at[r0], {"rep": r}).start()

    def forward(r):
        return remote(gath.at[t0, r], gath.at[t0, r], fs_.at[r], fr.at[r], {"tp": t1})

    def forwarded(r):
        return remote(gath.at[t1, r], gath.at[t1, r], fs_.at[r], fr.at[r], {"tp": t1})

    forward(r0).start()

    lax.fori_loop(1, F, sq1_wait, 0)
    acc = sq1[0]
    for f in range(1, F):
        acc = acc + sq1[f]
    slot = t0 * R + r0
    sq2[slot] = acc

    def sq2_copy(k, t, which):
        r, tp = lax.rem(r0 + k, R), lax.rem(t0 + t, 2)
        other = tp * R + r
        here = slot if which == 0 else other
        return remote(sq2.at[here], sq2.at[here], q2s.at[other], q2r.at[here], {"rep": r, "tp": tp})

    for k, t in group:
        sq2_copy(k, t, 0).start()

    for k in range(1, R):
        r = lax.rem(r0 + k, R)
        remote(gath.at[t0, r], gath.at[t0, r], gs.at[r], gr.at[r], {"rep": r}).wait_recv()
        forward(r).start()

    for k, t in group:
        sq2_copy(k, t, 1).wait_recv()
    acc = sq2[0]
    for i in range(1, 2 * R):
        acc = acc + sq2[i]
    total[...] = acc

    for k in range(R):
        forwarded(lax.rem(r0 + k, R)).wait_recv()

    swap.wait_send()

    def drain1(d, _):
        f = lax.rem(f0 + d, F)
        for k in range(1, R):
            copy1(f, k).wait_send()
        return 0

    lax.fori_loop(1, F + 1, drain1, 0)

    def drain2(d, _):
        f = lax.rem(f0 + d, F)
        remote(out2.at[f], land2.at[f0], s2.at[f], r2.at[f0], {"fs": f}).wait_send()
        sq1_copy(d).wait_send()
        return 0

    lax.fori_loop(1, F, drain2, 0)
    for k in range(1, R):
        r = lax.rem(r0 + k, R)
        remote(gath.at[t0, r0], gath.at[t0, r0], gs.at[r], gr.at[r0], {"rep": r}).wait_send()
    for k in range(R):
        forward(lax.rem(r0 + k, R)).wait_send()
    for k, t in group:
        sq2_copy(k, t, 0).wait_send()


def finish(
    count, R,
    gath, total, grad, kb, vb, kmast, vmast, km, ks, vm, vs,
    kmean, ksquare, vmean, vsquare, kstep, vstep, kweight, vweight,
):
    width = km.shape[1]

    @pl.when(pl.program_id(0) == 0)
    def _():
        kmean[...], ksquare[...] = moments(grad[:, :width], km[...], ks[...])
        vmean[...], vsquare[...] = moments(grad[:, width:], vm[...], vs[...])

    whole = jnp.sum(total[...], axis=1, keepdims=True)
    inverse = 1.0 / jnp.sqrt(whole / count + mean_epsilon)
    for h, (basis, master, step, weight) in enumerate(
        ((kb, kmast, kstep, kweight), (vb, vmast, vstep, vweight))
    ):
        rows = jnp.concatenate(
            [gath[t, 0, :, h * width:(h + 1) * width] for t in range(2)], axis=1
        )
        out = lax.dot_general(
            rows, basis[...], (((1,), (1,)), ((), ())), preferred_element_type=F32
        ) * inverse
        step[...] = out
        weight[...] = (master[...] - learn_rate * out).astype(BF16)


def shards(F, R, x, kc, vc, kb, vb, kmast, vmast, km, ks, vm, vs):
    rows, width = km.shape
    both = 2 * width
    tok, D = x.shape
    wire = BF16 if rows % 16 == 0 else F32
    any_ = pl.BlockSpec(memory_space=pl.ANY)
    vmem = pl.BlockSpec(memory_space=pltpu.VMEM)
    dma = pltpu.SemaphoreType.DMA
    staged = (x, kc, vc, kb, vb, km, ks, vm, vs)
    gath, total, grad = pl.pallas_call(
        functools.partial(exchange, F, R),
        out_shape=(
            jax.ShapeDtypeStruct((2, R, rows, both), BF16),
            jax.ShapeDtypeStruct((1, width), F32),
            jax.ShapeDtypeStruct((rows, both), F32),
        ),
        in_specs=[any_] * 9,
        out_specs=(vmem,) * 3,
        scratch_shapes=[pltpu.VMEM(a.shape, a.dtype) for a in staged] + [
            pltpu.VMEM((2, tok, both), F32),
            pltpu.VMEM((tok, both), F32),
            pltpu.VMEM((F, R, rows, both), wire),
            pltpu.VMEM((F, R, rows, both), wire),
            pltpu.VMEM((F, rows, both), wire),
            pltpu.VMEM((F, rows, both), wire),
            pltpu.VMEM((F, 1, width), F32),
            pltpu.VMEM((2 * R, 1, width), F32),
            dma((9,)), dma, dma, dma((F, R)), dma((F, R)), dma((F,)), dma((F,)),
            dma((R,)), dma((R,)), dma((R,)), dma((R,)),
            dma((F,)), dma((F,)), dma((2 * R,)), dma((2 * R,)),
        ],
        compiler_params=pltpu.CompilerParams(collective_id=0, has_side_effects=True),
        name="exchange",
    )(x, kc, vc, kb, vb, km, ks, vm, vs)

    def row(a):
        return pl.BlockSpec((rows, a.shape[1]), lambda i: (i, 0))

    def fixed(a):
        return pl.BlockSpec(a.shape, lambda i: (0,) * len(a.shape))

    sds = jax.ShapeDtypeStruct
    return pl.pallas_call(
        functools.partial(finish, 2 * D * both, R),
        grid=(R,),
        out_shape=tuple(sds(a.shape, F32) for a in (km, ks, vm, vs, kmast, vmast))
        + tuple(sds(a.shape, BF16) for a in (kmast, vmast)),
        in_specs=[
            pl.BlockSpec((2, 1, rows, both), lambda i: (0, i, 0, 0)),
            fixed(total), fixed(grad), fixed(kb), fixed(vb), row(kmast), row(vmast),
            fixed(km), fixed(ks), fixed(vm), fixed(vs),
        ],
        out_specs=(fixed(km), fixed(ks), fixed(vm), fixed(vs),
                   row(kmast), row(vmast), row(kmast), row(vmast)),
        name="finish",
    )(gath, total, grad, kb, vb, kmast, vmast, km, ks, vm, vs)


def solution(mesh):
    rows = ("fs", "rep")
    placed = (
        (P(rows, None),) + (P(rows, "tp"),) * 2 + (P("tp", None),) * 2
        + (P("fs", "tp"),) * 2 + (P(rows, "tp"),) * 4
    )
    return jax.shard_map(
        functools.partial(shards, mesh.shape["fs"], mesh.shape["rep"]),
        mesh=mesh,
        in_specs=placed,
        out_specs=(P(rows, "tp"),) * 4 + (P("fs", "tp"),) * 4,
        check_vma=False,
    )
```

```python
import functools

import jax
import jax.numpy as jnp
from jax import lax
from jax.experimental import pallas as pl
from jax.experimental.pallas import tpu as pltpu
from jax.sharding import PartitionSpec as P

first_decay = 0.8
second_decay = 0.9
root_epsilon = 1e-08
mean_epsilon = 1e-06
learn_rate = 0.01

F32 = jnp.float32
BF16 = jnp.bfloat16
MESH = pl.DeviceIdType.MESH


def moments(grad, moment, second):
    mean = first_decay * moment + (1.0 - first_decay) * grad
    square = second_decay * second + (1.0 - second_decay) * grad * grad
    return mean, square


def remote(src, dst, send, recv, where):
    return pltpu.make_async_remote_copy(
        src_ref=src, dst_ref=dst, send_sem=send, recv_sem=recv,
        device_id=where, device_id_type=MESH,
    )


def exchange(
    F, R,
    x_v, kc_v, vc_v, kb_v, vb_v, km_v, ks_v, vm_v, vs_v,
    gath, total, grad,
    proj, proj_in, part, land1, out2, land2, sq1, sq2,
    p_send, p_recv, s1, r1, s2, r2, gs, gr, fs_, fr, q1s, q1r, q2s, q2r,
):
    f0, r0, t0 = lax.axis_index("fs"), lax.axis_index("rep"), lax.axis_index("tp")
    t1 = 1 - t0
    D = x_v.shape[1]
    rows, width = km_v.shape
    wire = part.dtype

    barrier = pltpu.get_barrier_semaphore()

    def greet_fs(d, _):
        pl.semaphore_signal(barrier, inc=1, device_id={"fs": lax.rem(f0 + d, F)}, device_id_type=MESH)
        return 0

    lax.fori_loop(1, F, greet_fs, 0)
    group = [(k, t) for k in range(R) for t in range(2) if (k, t) != (0, 0)]
    for k, t in group:
        pl.semaphore_signal(
            barrier, inc=1,
            device_id={"rep": lax.rem(r0 + k, R), "tp": lax.rem(t0 + t, 2)},
            device_id_type=MESH,
        )

    pk = jnp.dot(kc_v[...], kb_v[...], preferred_element_type=F32)
    for t in range(2):
        proj[t, :, :width] = pk[:, t * width:(t + 1) * width]
    pv = jnp.dot(vc_v[...], vb_v[...], preferred_element_type=F32)
    for t in range(2):
        proj[t, :, width:] = pv[:, t * width:(t + 1) * width]

    pl.semaphore_wait(barrier, F - 1 + 2 * R - 1)
    swap = remote(proj.at[t1], proj_in, p_send, p_recv, {"tp": t1})
    swap.start()
    swap.wait_recv()
    joined = (proj[t0] + proj_in[...]).astype(BF16)

    tile = min(256, D)
    for i in range(D // tile):
        g = lax.dot_general(
            x_v[:, i * tile:(i + 1) * tile], joined, (((0,), (0,)), ((), ())),
            preferred_element_type=F32,
        )
        for c in range(tile // rows):
            at = i * (tile // rows) + c
            part[at // R, at % R] = g[c * rows:(c + 1) * rows].astype(wire)

    def copy1(f, k):
        r = lax.rem(r0 + k, R)
        return remote(part.at[f, r], land1.at[f, r0], s1.at[f, r], r1.at[f, r0], {"rep": r})

    def wait1(f, k):
        r = lax.rem(r0 + k, R)
        remote(part.at[f, r], land1.at[f, r], s1.at[f, r], r1.at[f, r], {"rep": r}).wait_recv()

    def send1(d, _):
        f = lax.rem(f0 + d, F)
        for k in range(1, R):
            copy1(f, k).start()
        return 0

    lax.fori_loop(1, F + 1, send1, 0)

    def gather1(f):
        acc = part[f, r0].astype(F32)
        for k in range(1, R):
            wait1(f, k)
            acc = acc + land1[f, lax.rem(r0 + k, R)].astype(F32)
        return acc

    def send2(d, _):
        f = lax.rem(f0 + d, F)
        out2[f] = gather1(f).astype(wire)
        remote(out2.at[f], land2.at[f0], s2.at[f], r2.at[f0], {"fs": f}).start()
        return 0

    lax.fori_loop(1, F, send2, 0)
    grad[...] = gather1(f0)

    def add2(d, _):
        f = lax.rem(f0 + d, F)
        remote(out2.at[f], land2.at[f], s2.at[f], r2.at[f], {"fs": f}).wait_recv()
        grad[...] += land2[f].astype(F32)
        return 0

    lax.fori_loop(1, F, add2, 0)

    squares = 0.0
    for h, (m_v, s_v) in enumerate(((km_v, ks_v), (vm_v, vs_v))):
        mean, square = moments(grad[:, h * width:(h + 1) * width], m_v[...], s_v[...])
        ratio = mean / (jnp.sqrt(square) + root_epsilon)
        gath[t0, r0, :, h * width:(h + 1) * width] = ratio.astype(BF16)
        squares = squares + jnp.sum(ratio * ratio, axis=0, keepdims=True)
    sq1[f0] = squares

    def sq1_copy(d):
        f = lax.rem(f0 + d, F)
        return remote(sq1.at[f0], sq1.at[f0], q1s.at[f], q1r.at[f0], {"fs": f})

    def sq1_wait(d, acc):
        f = lax.rem(f0 + d, F)
        remote(sq1.at[f], sq1.at[f], q1s.at[f], q1r.at[f], {"fs": f}).wait_recv()
        return acc

    def sq1_start(d, _):
        sq1_copy(d).start()
        return 0

    lax.fori_loop(1, F, sq1_start, 0)

    for k in range(1, R):
        r = lax.rem(r0 + k, R)
        remote(gath.at[t0, r0], gath.at[t0, r0], gs.at[r], gr.at[r0], {"rep": r}).start()

    def forward(r):
        return remote(gath.at[t0, r], gath.at[t0, r], fs_.at[r], fr.at[r], {"tp": t1})

    def forwarded(r):
        return remote(gath.at[t1, r], gath.at[t1, r], fs_.at[r], fr.at[r], {"tp": t1})

    forward(r0).start()

    lax.fori_loop(1, F, sq1_wait, 0)
    acc = sq1[0]
    for f in range(1, F):
        acc = acc + sq1[f]
    slot = t0 * R + r0
    sq2[slot] = acc

    def sq2_copy(k, t, which):
        r, tp = lax.rem(r0 + k, R), lax.rem(t0 + t, 2)
        other = tp * R + r
        here = slot if which == 0 else other
        return remote(sq2.at[here], sq2.at[here], q2s.at[other], q2r.at[here], {"rep": r, "tp": tp})

    for k, t in group:
        sq2_copy(k, t, 0).start()

    for k in range(1, R):
        r = lax.rem(r0 + k, R)
        remote(gath.at[t0, r], gath.at[t0, r], gs.at[r], gr.at[r], {"rep": r}).wait_recv()
        forward(r).start()

    for k, t in group:
        sq2_copy(k, t, 1).wait_recv()
    acc = sq2[0]
    for i in range(1, 2 * R):
        acc = acc + sq2[i]
    total[...] = acc

    for k in range(R):
        forwarded(lax.rem(r0 + k, R)).wait_recv()

    swap.wait_send()

    def drain1(d, _):
        f = lax.rem(f0 + d, F)
        for k in range(1, R):
            copy1(f, k).wait_send()
        return 0

    lax.fori_loop(1, F + 1, drain1, 0)

    def drain2(d, _):
        f = lax.rem(f0 + d, F)
        remote(out2.at[f], land2.at[f0], s2.at[f], r2.at[f0], {"fs": f}).wait_send()
        sq1_copy(d).wait_send()
        return 0

    lax.fori_loop(1, F, drain2, 0)
    for k in range(1, R):
        r = lax.rem(r0 + k, R)
        remote(gath.at[t0, r0], gath.at[t0, r0], gs.at[r], gr.at[r0], {"rep": r}).wait_send()
    for k in range(R):
        forward(lax.rem(r0 + k, R)).wait_send()
    for k, t in group:
        sq2_copy(k, t, 0).wait_send()


def finish(
    count, R,
    gath, total, grad, kb, vb, kmast, vmast, km, ks, vm, vs,
    kmean, ksquare, vmean, vsquare, kstep, vstep, kweight, vweight,
):
    width = km.shape[1]

    @pl.when(pl.program_id(0) == 0)
    def _():
        kmean[...], ksquare[...] = moments(grad[:, :width], km[...], ks[...])
        vmean[...], vsquare[...] = moments(grad[:, width:], vm[...], vs[...])

    whole = jnp.sum(total[...], axis=1, keepdims=True)
    inverse = 1.0 / jnp.sqrt(whole / count + mean_epsilon)
    for h, (basis, master, step, weight) in enumerate(
        ((kb, kmast, kstep, kweight), (vb, vmast, vstep, vweight))
    ):
        rows = jnp.concatenate(
            [gath[t, 0, :, h * width:(h + 1) * width] for t in range(2)], axis=1
        )
        out = lax.dot_general(
            rows, basis[...], (((1,), (1,)), ((), ())), preferred_element_type=F32
        ) * inverse
        step[...] = out
        weight[...] = (master[...] - learn_rate * out).astype(BF16)


def shards(F, R, x, kc, vc, kb, vb, kmast, vmast, km, ks, vm, vs):
    rows, width = km.shape
    both = 2 * width
    tok, D = x.shape
    wire = BF16 if rows % 16 == 0 else F32
    vmem = pl.BlockSpec(memory_space=pltpu.VMEM)
    dma = pltpu.SemaphoreType.DMA
    gath, total, grad = pl.pallas_call(
        functools.partial(exchange, F, R),
        out_shape=(
            jax.ShapeDtypeStruct((2, R, rows, both), BF16),
            jax.ShapeDtypeStruct((1, width), F32),
            jax.ShapeDtypeStruct((rows, both), F32),
        ),
        in_specs=[vmem] * 9,
        out_specs=(vmem,) * 3,
        scratch_shapes=[
            pltpu.VMEM((2, tok, both), F32),
            pltpu.VMEM((tok, both), F32),
            pltpu.VMEM((F, R, rows, both), wire),
            pltpu.VMEM((F, R, rows, both), wire),
            pltpu.VMEM((F, rows, both), wire),
            pltpu.VMEM((F, rows, both), wire),
            pltpu.VMEM((F, 1, width), F32),
            pltpu.VMEM((2 * R, 1, width), F32),
            dma, dma, dma((F, R)), dma((F, R)), dma((F,)), dma((F,)),
            dma((R,)), dma((R,)), dma((R,)), dma((R,)),
            dma((F,)), dma((F,)), dma((2 * R,)), dma((2 * R,)),
        ],
        compiler_params=pltpu.CompilerParams(
            collective_id=0, has_side_effects=True, vmem_limit_bytes=14 << 20
        ),
        cost_estimate=pl.CostEstimate(
            flops=4 * tok * D * both, bytes_accessed=200 * x.size, transcendentals=0
        ),
        name="exchange",
    )(x, kc, vc, kb, vb, km, ks, vm, vs)

    def row(a):
        return pl.BlockSpec((rows, a.shape[1]), lambda i: (i, 0))

    def fixed(a):
        return pl.BlockSpec(a.shape, lambda i: (0,) * len(a.shape))

    sds = jax.ShapeDtypeStruct
    return pl.pallas_call(
        functools.partial(finish, 2 * D * kb.shape[1], R),
        grid=(R,),
        out_shape=tuple(sds(a.shape, F32) for a in (km, ks, vm, vs, kmast, vmast))
        + tuple(sds(a.shape, BF16) for a in (kmast, vmast)),
        in_specs=[
            pl.BlockSpec((2, 1, rows, both), lambda i: (0, i, 0, 0)),
            fixed(total), fixed(grad), fixed(kb), fixed(vb), row(kmast), row(vmast),
            fixed(km), fixed(ks), fixed(vm), fixed(vs),
        ],
        out_specs=(fixed(km), fixed(ks), fixed(vm), fixed(vs),
                   row(kmast), row(vmast), row(kmast), row(vmast)),
        compiler_params=pltpu.CompilerParams(vmem_limit_bytes=16 << 20),
        cost_estimate=pl.CostEstimate(
            flops=2 * R * rows * both * (kmast.shape[1] + vmast.shape[1]),
            bytes_accessed=10 * (kmast.size + vmast.size), transcendentals=0,
        ),
        name="finish",
    )(gath, total, grad, kb, vb, kmast, vmast, km, ks, vm, vs)


def solution(mesh):
    rows = ("fs", "rep")
    placed = (
        (P(rows, None),) + (P(rows, "tp"),) * 2 + (P("tp", None),) * 2
        + (P("fs", "tp"),) * 2 + (P(rows, "tp"),) * 4
    )
    return jax.shard_map(
        functools.partial(shards, mesh.shape["fs"], mesh.shape["rep"]),
        mesh=mesh,
        in_specs=placed,
        out_specs=(P(rows, "tp"),) * 4 + (P("fs", "tp"),) * 4,
        check_vma=False,
    )
```

```python
import functools

import jax
import jax.numpy as jnp
from jax import lax
from jax.experimental import pallas as pl
from jax.experimental.pallas import tpu as pltpu
from jax.sharding import PartitionSpec as P

first_decay = 0.8
second_decay = 0.9
root_epsilon = 1e-08
mean_epsilon = 1e-06
learn_rate = 0.01

F32 = jnp.float32
BF16 = jnp.bfloat16
MESH = pl.DeviceIdType.MESH


def moments(grad, moment, second):
    mean = first_decay * moment + (1.0 - first_decay) * grad
    square = second_decay * second + (1.0 - second_decay) * grad * grad
    return mean, square


def remote(src, dst, send, recv, where):
    return pltpu.make_async_remote_copy(
        src_ref=src, dst_ref=dst, send_sem=send, recv_sem=recv,
        device_id=where, device_id_type=MESH,
    )


def exchange(
    F, R,
    x, kc, vc, kb, vb, km, ks, vm, vs,
    gath, total, grad,
    x_v, kc_v, vc_v, kb_v, vb_v, km_v, ks_v, vm_v, vs_v,
    proj, proj_in, part, land1, out2, land2, sq1, sq2,
    load, p_send, p_recv, s1, r1, s2, r2, gs, gr, fs_, fr, q1s, q1r, q2s, q2r,
):
    f0, r0, t0 = lax.axis_index("fs"), lax.axis_index("rep"), lax.axis_index("tp")
    t1 = 1 - t0
    D = x.shape[1]
    rows, width = km.shape
    wire = part.dtype

    pairs = [(kc, kc_v), (kb, kb_v), (vc, vc_v), (vb, vb_v), (x, x_v),
             (km, km_v), (ks, ks_v), (vm, vm_v), (vs, vs_v)]
    loads = [pltpu.make_async_copy(a, b, load.at[i]) for i, (a, b) in enumerate(pairs)]
    for c in loads:
        c.start()

    barrier = pltpu.get_barrier_semaphore()

    def greet_fs(d, _):
        pl.semaphore_signal(barrier, inc=1, device_id={"fs": lax.rem(f0 + d, F)}, device_id_type=MESH)
        return 0

    lax.fori_loop(1, F, greet_fs, 0)
    group = [(k, t) for k in range(R) for t in range(2) if (k, t) != (0, 0)]
    for k, t in group:
        pl.semaphore_signal(
            barrier, inc=1,
            device_id={"rep": lax.rem(r0 + k, R), "tp": lax.rem(t0 + t, 2)},
            device_id_type=MESH,
        )

    for c in loads[:2]:
        c.wait()
    pk = jnp.dot(kc_v[...], kb_v[...], preferred_element_type=F32)
    for t in range(2):
        proj[t, :, :width] = pk[:, t * width:(t + 1) * width]
    for c in loads[2:4]:
        c.wait()
    pv = jnp.dot(vc_v[...], vb_v[...], preferred_element_type=F32)
    for t in range(2):
        proj[t, :, width:] = pv[:, t * width:(t + 1) * width]

    pl.semaphore_wait(barrier, F - 1 + 2 * R - 1)
    swap = remote(proj.at[t1], proj_in, p_send, p_recv, {"tp": t1})
    swap.start()
    loads[4].wait()
    swap.wait_recv()
    joined = (proj[t0] + proj_in[...]).astype(BF16)

    def copy1(f, k):
        r = lax.rem(r0 + k, R)
        return remote(part.at[f, r], land1.at[f, r0], s1.at[f, r], r1.at[f, r0], {"rep": r})

    def wait1(f, k):
        r = lax.rem(r0 + k, R)
        remote(part.at[f, r], land1.at[f, r], s1.at[f, r], r1.at[f, r], {"rep": r}).wait_recv()

    def send1(d, _):
        f = lax.rem(f0 + d, F)
        for k in range(1, R):
            copy1(f, k).start()
        return 0

    span = R * rows
    if span % 256 == 0 and 256 % rows == 0:
        def make_and_send(d, _):
            f = lax.rem(f0 + d, F)
            for i in range(span // 256):
                at = pl.multiple_of(f * span + i * 256, 256)
                g = lax.dot_general(
                    x_v[:, pl.ds(at, 256)], joined, (((0,), (0,)), ((), ())),
                    preferred_element_type=F32,
                )
                for c in range(256 // rows):
                    part[f, i * (256 // rows) + c] = g[c * rows:(c + 1) * rows].astype(wire)
            return send1(d, 0)

        lax.fori_loop(1, F + 1, make_and_send, 0, unroll=True)
    else:
        tile = min(256, D)
        for i in range(D // tile):
            g = lax.dot_general(
                x_v[:, i * tile:(i + 1) * tile], joined, (((0,), (0,)), ((), ())),
                preferred_element_type=F32,
            )
            for c in range(tile // rows):
                at = i * (tile // rows) + c
                part[at // R, at % R] = g[c * rows:(c + 1) * rows].astype(wire)
        lax.fori_loop(1, F + 1, send1, 0)

    def gather1(f):
        acc = part[f, r0].astype(F32)
        for k in range(1, R):
            wait1(f, k)
            acc = acc + land1[f, lax.rem(r0 + k, R)].astype(F32)
        return acc

    def send2(d, _):
        f = lax.rem(f0 + d, F)
        out2[f] = gather1(f).astype(wire)
        remote(out2.at[f], land2.at[f0], s2.at[f], r2.at[f0], {"fs": f}).start()
        return 0

    lax.fori_loop(1, F, send2, 0)
    for c in loads[5:]:
        c.wait()
    grad[...] = gather1(f0)

    def add2(d, _):
        f = lax.rem(f0 + d, F)
        remote(out2.at[f], land2.at[f], s2.at[f], r2.at[f], {"fs": f}).wait_recv()
        grad[...] += land2[f].astype(F32)
        return 0

    lax.fori_loop(1, F, add2, 0)

    squares = 0.0
    for h, (m_v, s_v) in enumerate(((km_v, ks_v), (vm_v, vs_v))):
        mean, square = moments(grad[:, h * width:(h + 1) * width], m_v[...], s_v[...])
        ratio = mean / (jnp.sqrt(square) + root_epsilon)
        gath[t0, r0, :, h * width:(h + 1) * width] = ratio.astype(BF16)
        squares = squares + jnp.sum(ratio * ratio, axis=0, keepdims=True)
    sq1[f0] = squares

    def sq1_copy(d):
        f = lax.rem(f0 + d, F)
        return remote(sq1.at[f0], sq1.at[f0], q1s.at[f], q1r.at[f0], {"fs": f})

    def sq1_wait(d, acc):
        f = lax.rem(f0 + d, F)
        remote(sq1.at[f], sq1.at[f], q1s.at[f], q1r.at[f], {"fs": f}).wait_recv()
        return acc

    def sq1_start(d, _):
        sq1_copy(d).start()
        return 0

    lax.fori_loop(1, F, sq1_start, 0)

    for k in range(1, R):
        r = lax.rem(r0 + k, R)
        remote(gath.at[t0, r0], gath.at[t0, r0], gs.at[r], gr.at[r0], {"rep": r}).start()

    def forward(r):
        return remote(gath.at[t0, r], gath.at[t0, r], fs_.at[r], fr.at[r], {"tp": t1})

    def forwarded(r):
        return remote(gath.at[t1, r], gath.at[t1, r], fs_.at[r], fr.at[r], {"tp": t1})

    forward(r0).start()

    lax.fori_loop(1, F, sq1_wait, 0)
    acc = sq1[0]
    for f in range(1, F):
        acc = acc + sq1[f]
    slot = t0 * R + r0
    sq2[slot] = acc

    def sq2_copy(k, t, which):
        r, tp = lax.rem(r0 + k, R), lax.rem(t0 + t, 2)
        other = tp * R + r
        here = slot if which == 0 else other
        return remote(sq2.at[here], sq2.at[here], q2s.at[other], q2r.at[here], {"rep": r, "tp": tp})

    for k, t in group:
        sq2_copy(k, t, 0).start()

    for k in range(1, R):
        r = lax.rem(r0 + k, R)
        remote(gath.at[t0, r], gath.at[t0, r], gs.at[r], gr.at[r], {"rep": r}).wait_recv()
        forward(r).start()

    for k, t in group:
        sq2_copy(k, t, 1).wait_recv()
    acc = sq2[0]
    for i in range(1, 2 * R):
        acc = acc + sq2[i]
    total[...] = acc

    for k in range(R):
        forwarded(lax.rem(r0 + k, R)).wait_recv()

    swap.wait_send()

    def drain1(d, _):
        f = lax.rem(f0 + d, F)
        for k in range(1, R):
            copy1(f, k).wait_send()
        return 0

    lax.fori_loop(1, F + 1, drain1, 0)

    def drain2(d, _):
        f = lax.rem(f0 + d, F)
        remote(out2.at[f], land2.at[f0], s2.at[f], r2.at[f0], {"fs": f}).wait_send()
        sq1_copy(d).wait_send()
        return 0

    lax.fori_loop(1, F, drain2, 0)
    for k in range(1, R):
        r = lax.rem(r0 + k, R)
        remote(gath.at[t0, r0], gath.at[t0, r0], gs.at[r], gr.at[r0], {"rep": r}).wait_send()
    for k in range(R):
        forward(lax.rem(r0 + k, R)).wait_send()
    for k, t in group:
        sq2_copy(k, t, 0).wait_send()


def finish(
    count, R,
    gath, total, grad, kb, vb, kmast, vmast, km, ks, vm, vs,
    kmean, ksquare, vmean, vsquare, kstep, vstep, kweight, vweight,
):
    width = km.shape[1]

    @pl.when(pl.program_id(0) == 0)
    def _():
        kmean[...], ksquare[...] = moments(grad[:, :width], km[...], ks[...])
        vmean[...], vsquare[...] = moments(grad[:, width:], vm[...], vs[...])

    whole = jnp.sum(total[...], axis=1, keepdims=True)
    inverse = 1.0 / jnp.sqrt(whole / count + mean_epsilon)
    for h, (basis, master, step, weight) in enumerate(
        ((kb, kmast, kstep, kweight), (vb, vmast, vstep, vweight))
    ):
        rows = jnp.concatenate(
            [gath[t, 0, :, h * width:(h + 1) * width] for t in range(2)], axis=1
        )
        out = lax.dot_general(
            rows, basis[...], (((1,), (1,)), ((), ())), preferred_element_type=F32
        ) * inverse
        step[...] = out
        weight[...] = (master[...] - learn_rate * out).astype(BF16)


def shards(F, R, x, kc, vc, kb, vb, kmast, vmast, km, ks, vm, vs):
    rows, width = km.shape
    both = 2 * width
    tok, D = x.shape
    wire = BF16 if rows % 16 == 0 else F32
    any_ = pl.BlockSpec(memory_space=pl.ANY)
    vmem = pl.BlockSpec(memory_space=pltpu.VMEM)
    dma = pltpu.SemaphoreType.DMA
    staged = (x, kc, vc, kb, vb, km, ks, vm, vs)
    gath, total, grad = pl.pallas_call(
        functools.partial(exchange, F, R),
        out_shape=(
            jax.ShapeDtypeStruct((2, R, rows, both), BF16),
            jax.ShapeDtypeStruct((1, width), F32),
            jax.ShapeDtypeStruct((rows, both), F32),
        ),
        in_specs=[any_] * 9,
        out_specs=(vmem,) * 3,
        scratch_shapes=[pltpu.VMEM(a.shape, a.dtype) for a in staged] + [
            pltpu.VMEM((2, tok, both), F32),
            pltpu.VMEM((tok, both), F32),
            pltpu.VMEM((F, R, rows, both), wire),
            pltpu.VMEM((F, R, rows, both), wire),
            pltpu.VMEM((F, rows, both), wire),
            pltpu.VMEM((F, rows, both), wire),
            pltpu.VMEM((F, 1, width), F32),
            pltpu.VMEM((2 * R, 1, width), F32),
            dma((9,)), dma, dma, dma((F, R)), dma((F, R)), dma((F,)), dma((F,)),
            dma((R,)), dma((R,)), dma((R,)), dma((R,)),
            dma((F,)), dma((F,)), dma((2 * R,)), dma((2 * R,)),
        ],
        compiler_params=pltpu.CompilerParams(collective_id=0, has_side_effects=True),
        name="exchange",
    )(x, kc, vc, kb, vb, km, ks, vm, vs)

    def row(a):
        return pl.BlockSpec((rows, a.shape[1]), lambda i: (i, 0))

    def fixed(a):
        return pl.BlockSpec(a.shape, lambda i: (0,) * len(a.shape))

    sds = jax.ShapeDtypeStruct
    return pl.pallas_call(
        functools.partial(finish, 2 * D * both, R),
        grid=(R,),
        out_shape=tuple(sds(a.shape, F32) for a in (km, ks, vm, vs, kmast, vmast))
        + tuple(sds(a.shape, BF16) for a in (kmast, vmast)),
        in_specs=[
            pl.BlockSpec((2, 1, rows, both), lambda i: (0, i, 0, 0)),
            fixed(total), fixed(grad), fixed(kb), fixed(vb), row(kmast), row(vmast),
            fixed(km), fixed(ks), fixed(vm), fixed(vs),
        ],
        out_specs=(fixed(km), fixed(ks), fixed(vm), fixed(vs),
                   row(kmast), row(vmast), row(kmast), row(vmast)),
        name="finish",
    )(gath, total, grad, kb, vb, kmast, vmast, km, ks, vm, vs)


def solution(mesh):
    rows = ("fs", "rep")
    placed = (
        (P(rows, None),) + (P(rows, "tp"),) * 2 + (P("tp", None),) * 2
        + (P("fs", "tp"),) * 2 + (P(rows, "tp"),) * 4
    )
    return jax.shard_map(
        functools.partial(shards, mesh.shape["fs"], mesh.shape["rep"]),
        mesh=mesh,
        in_specs=placed,
        out_specs=(P(rows, "tp"),) * 4 + (P("fs", "tp"),) * 4,
        check_vma=False,
    )
```
